32 devices in a mesh: ep: 8 (over z, x), tp: 4 (over y, core).
Axes of the slice: x: 2, y: 2, z: 4, core: 2. Of those that a mesh axis runs over, the one named last changes fastest.
Arguments:
- tokens: bfloat16 [128, 2048], P('ep'), may hold values from -6 to 6
- lengths: int32 [128], P('ep'), may hold values from 1024 to 16384
- old_state: float32 [128, 8, 128, 128], P('ep', 'tp'), may hold values from -2 to 2
- query_weight: bfloat16 [2048, 1024], P(None, 'tp'), may hold values from -0.125 to 0.125
- key_weight: bfloat16 [2048, 1024], P(None, 'tp'), may hold values from -0.125 to 0.125
- value_weight: bfloat16 [2048, 1024], P(None, 'tp'), may hold values from -0.125 to 0.125
- gate_weight: bfloat16 [2048, 1024], P(None, 'tp'), may hold values from -0.125 to 0.125
- head_gain: float32 [1024], P('tp'), may hold values from 0.1 to 1.9
- output_weight: bfloat16 [1024, 2048], P('tp'), may hold values from -0.1875 to 0.1875
- first_gain: float32 [2048], replicated, may hold values from 0.1 to 1.9
- expert_ids: int32 [128, 6], P('ep'), may hold values from 0 to 15, all different within a row; in each aligned block of 16 rows (0 to 15, 16 to 31, ...) at most 7 rows name the same one
- expert_weights: float32 [128, 6], P('ep'), may hold values from 0.05 to 0.8
- expert_gate: bfloat16 [16, 2048, 512], P('ep', None, 'tp'), may hold values from -0.125 to 0.125
- expert_up: bfloat16 [16, 2048, 512], P('ep', None, 'tp'), may hold values from -0.125 to 0.125
- expert_down: bfloat16 [16, 512, 2048], P('ep', 'tp'), may hold values from -0.25 to 0.25
- shared_gate: bfloat16 [2048, 512], P(None, 'tp'), may hold values from -0.125 to 0.125
- shared_up: bfloat16 [2048, 512], P(None, 'tp'), may hold values from -0.125 to 0.125
- shared_down: bfloat16 [512, 2048], P('tp'), may hold values from -0.25 to 0.25
- side_gate: bfloat16 [2048], replicated, may hold values from -0.125 to 0.125
- dense_gate: bfloat16 [2048, 8192], P(None, ('ep', 'tp')), may hold values from -0.125 to 0.125
- dense_up: bfloat16 [2048, 8192], P(None, ('ep', 'tp')), may hold values from -0.125 to 0.125
- dense_down: bfloat16 [8192, 2048], P(('ep', 'tp')), may hold values from -0.25 to 0.25
- second_gain: float32 [2048], replicated, may hold values from 0.1 to 1.9
Outputs:
- layer_out: bfloat16 [128, 2048], P('ep')
- new_state: float32 [128, 8, 128, 128], P('ep', 'tp')
The draws below stay inside these ranges and needn't reach their ends.
Inputs may be any that keep to these rules, and one draw needn't show every extreme that they name: `expert_ids`: each row names 6 different experts. Among the 16 rows of one index of ep no expert is named by more than 7 rows, a bound that some block reaches.
All inputs are finite; a program needn't handle non-finite values.
Results may differ from the reference program's by a relative error of at most 0.017.
Values may be sent and summed in bfloat16 or wider, within the bound.
A program may use at most 64 MiB of HBM per device.

```python
import math
import jax
import jax.numpy as jnp
import numpy as np
from jax import lax

D = 2048
HEADS = 8
HD = 128
EFF = 512
SFF = 512
DENSE_FF = 8192
TOPK = 6
SEQ_DEV = 16
EXPERTS = 16
TOKENS = 128
CAP = 7
N_EP = 8
N_TP = 4


def set_ends(array, stream_key, low, high):
    extent = array.shape
    spot = [jax.random.randint(jax.random.fold_in(stream_key, axis), (), 0, extent[axis]) for axis in range(len(extent))]
    array = array.at[tuple(spot)].set(low)
    longest = extent.index(max(extent))
    spot[longest] = (spot[longest] + 1) % extent[longest]
    return array.at[tuple(spot)].set(high)


def levels(rng, extent, cuts, low, largest):
    gain, own = 1.0, jax.random.fold_in(rng, 6)
    for dim, parts in cuts:
        draws = jnp.exp(jax.random.uniform(jax.random.fold_in(own, dim), (parts,), jnp.float32, low / len(cuts), largest / len(cuts)))
        gain = gain * jnp.repeat(draws, extent[dim] // parts).reshape([-1 if axis == dim else 1 for axis in range(len(extent))])
    return gain


def deal_out(own_key, own, number, rows, amount, top, reach, lean):
    ranking = jax.random.permutation(own_key, amount)
    crowded, ordinary = shares(amount, rows * top, reach, lean, True), shares(amount, rows * top, reach, lean, False)
    places = jnp.arange(amount)

    def named(sizes, turn):
        used = int((sizes > 0).sum())
        fixed = max(1, used // 4)
        moved = fixed + (places - fixed + turn * (used - fixed)) % max(1, amount - fixed)
        return jnp.zeros((amount,), jnp.int32).at[ranking[jnp.where(places < fixed, places, moved)]].set(jnp.asarray(sizes, jnp.int32))

    sizes = jnp.where(number % 4 == 0, named(crowded, number // 4), named(ordinary, number - number // 4 - 1))
    mixed = jax.random.permutation(jax.random.fold_in(own, 3), amount)
    donor, receiver = mixed[0:amount // 2 * 2:2], mixed[1:amount // 2 * 2:2]
    margin = jnp.minimum(sizes[donor] - 1, reach - sizes[receiver]) // 2
    margin = jnp.where((donor == ranking[0]) | (receiver == ranking[0]) | (sizes[receiver] == 0), 0, jnp.maximum(margin, 0))
    moved = jax.random.randint(jax.random.fold_in(own, 4), (amount // 2,), 0, 1 << 20) % (margin + 1)
    sizes = sizes.at[donor].add(-moved).at[receiver].add(moved)
    items = jnp.searchsorted(jnp.cumsum(sizes), jnp.arange(rows * top), side="right").astype(jnp.int32)
    listing = items.reshape(top, rows).T
    listing = listing[jax.random.permutation(jax.random.fold_in(own, 1), rows)]
    turn = jax.random.randint(jax.random.fold_in(own, 2), (rows, 1), 0, top)
    return jnp.take_along_axis(listing, (jnp.arange(top)[None, :] + turn) % top, axis=1)


def shares(number_of, total, limit, lean, full):
    weights = [(1 << 20) // math.isqrt(standing ** lean) + 1 for standing in range(1, number_of + 1)]
    largest = limit if full else min(limit, max(-(-total // number_of), total * weights[0] // sum(weights)))
    least = 1 if total - largest >= number_of - 1 else 0
    counts, spare = [largest] + [least] * (number_of - 1), total - largest - least * (number_of - 1)
    while spare > 0:
        free = [i for i in range(1, number_of) if counts[i] < largest] or [i for i in range(1, number_of) if counts[i] < limit]
        pool, left = sum([weights[i] for i in free]), spare
        for i in free:
            extra = min(limit - counts[i], max(1, left * weights[i] // pool), spare)
            counts[i] = counts[i] + extra
            spare = spare - extra
    return np.array(counts)


def scatter_about(key, dims, width, limit, shards=(), held_as=jnp.bfloat16):
    factor_of = levels(key, dims, shards, -0.22, 0.18) if shards else 1.0
    drawn = jax.random.normal(key, dims, jnp.float32) * width * factor_of
    return jnp.minimum(jnp.maximum(drawn, -limit), limit).astype(held_as)


def setup_inputs(seed: int = 0) -> dict:
    key_of = jax.random.split(jax.random.key(seed), 24)
    tokens = scatter_about(key_of[0], (TOKENS, D), 1.0, 6.0, ((0, 8),))
    lengths = set_ends(jax.random.randint(key_of[1], (TOKENS,), 1024, 16385), jax.random.fold_in(key_of[1], 1), 1024, 16384).astype(jnp.int32)
    old_state = scatter_about(key_of[2], (TOKENS, HEADS, HD, HD), 0.25, 2.0, ((0, 8), (1, 4)), jnp.float32)
    query_weight = scatter_about(key_of[3], (D, HEADS * HD), D ** -0.5, 0.125, ((1, 4),))
    key_weight = scatter_about(key_of[4], (D, HEADS * HD), D ** -0.5, 0.125, ((1, 4),))
    value_weight = scatter_about(key_of[5], (D, HEADS * HD), D ** -0.5, 0.125, ((1, 4),))
    gate_weight = scatter_about(key_of[6], (D, HEADS * HD), D ** -0.5, 0.125, ((1, 4),))
    head_gain = jnp.clip(1.0 + 0.18 * jax.random.normal(key_of[7], (HEADS * HD,), jnp.float32), 0.1, 1.9)
    output_weight = scatter_about(key_of[8], (HEADS * HD, D), (HEADS * HD) ** -0.5, 0.1875, ((0, 4),))
    first_gain = jnp.clip(1.0 + 0.18 * jax.random.normal(key_of[9], (D,), jnp.float32), 0.1, 1.9)
    expert_ids_keys = jax.random.split(jax.random.fold_in(key_of[10], 1), TOKENS // SEQ_DEV)
    expert_ids_turns = jax.random.permutation(jax.random.fold_in(key_of[10], 3), TOKENS // SEQ_DEV)
    expert_ids = jax.vmap(lambda own, number: deal_out(jax.random.fold_in(key_of[10], 2), own, number, SEQ_DEV, EXPERTS, TOPK, CAP, 2))(expert_ids_keys, expert_ids_turns).reshape((TOKENS, TOPK))
    expert_weights = jnp.clip(jnp.exp(math.log(0.8) - 2.7725887 * jax.random.uniform(key_of[11], (TOKENS, TOPK), jnp.float32) ** levels(key_of[11], (TOKENS, TOPK), ((0, 8),), -0.2, 0.2)), 0.05, 0.8)
    expert_gate = scatter_about(key_of[12], (EXPERTS, D, EFF), D ** -0.5, 0.125, ((0, 8), (2, 4)))
    expert_up = scatter_about(key_of[13], (EXPERTS, D, EFF), D ** -0.5, 0.125, ((0, 8), (2, 4)))
    expert_down = scatter_about(key_of[14], (EXPERTS, EFF, D), EFF ** -0.5, 0.25, ((0, 8), (1, 4)))
    shared_gate = scatter_about(key_of[15], (D, SFF), D ** -0.5, 0.125, ((1, 4),))
    shared_up = scatter_about(key_of[16], (D, SFF), D ** -0.5, 0.125, ((1, 4),))
    shared_down = scatter_about(key_of[17], (SFF, D), SFF ** -0.5, 0.25, ((0, 4),))
    side_gate = scatter_about(key_of[18], (D,), D ** -0.5, 0.125)
    dense_gate = scatter_about(key_of[19], (D, DENSE_FF), D ** -0.5, 0.125, ((1, 32),))
    dense_up = scatter_about(key_of[20], (D, DENSE_FF), D ** -0.5, 0.125, ((1, 32),))
    dense_down = scatter_about(key_of[21], (DENSE_FF, D), (DENSE_FF // 16) ** -0.5, 0.25, ((0, 32),))
    second_gain = jnp.clip(1.0 + 0.18 * jax.random.normal(key_of[22], (D,), jnp.float32), 0.1, 1.9)
    return {"tokens": tokens, "lengths": lengths, "old_state": old_state, "query_weight": query_weight, "key_weight": key_weight, "value_weight": value_weight, "gate_weight": gate_weight, "head_gain": head_gain, "output_weight": output_weight, "first_gain": first_gain, "expert_ids": expert_ids, "expert_weights": expert_weights, "expert_gate": expert_gate, "expert_up": expert_up, "expert_down": expert_down, "shared_gate": shared_gate, "shared_up": shared_up, "shared_down": shared_down, "side_gate": side_gate, "dense_gate": dense_gate, "dense_up": dense_up, "dense_down": dense_down, "second_gain": second_gain}


NORM_EPS = 1e-05
RESIDUAL_SCALE = 2.0 ** 0.5

def rotate(inputs, positions):
    half_size = inputs.shape[-1] // 2
    frequency = 1.0 / 10000.0 ** (jnp.arange(half_size, dtype=jnp.float32) * 2.0 / inputs.shape[-1])
    angles = positions.astype(jnp.float32)[:, None] * frequency[None, :]
    cosine = jnp.cos(angles)[:, None, :]
    sine_part = jnp.sin(angles)[:, None, :]
    first_half = inputs[..., :half_size]
    second_half = inputs[..., half_size:]
    return jnp.concatenate([first_half * cosine - second_half * sine_part, first_half * sine_part + second_half * cosine], axis=-1)

def layer_norm(inputs, scale_gain):
    average = lax.optimization_barrier(jnp.mean(inputs, axis=-1, keepdims=True))
    centered = inputs - average
    variance = lax.optimization_barrier(jnp.mean(centered * centered, axis=-1, keepdims=True))
    return centered * lax.rsqrt(variance + NORM_EPS) * scale_gain

def reference(tokens, lengths, old_state, query_weight, key_weight, value_weight, gate_weight, head_gain, output_weight, first_gain, expert_ids, expert_weights, expert_gate, expert_up, expert_down, shared_gate, shared_up, shared_down, side_gate, dense_gate, dense_up, dense_down, second_gain):
    row_count = tokens.shape[0]
    head_count = old_state.shape[1]
    head_size = old_state.shape[-1]
    model_width = tokens.shape[1]
    queries = jnp.dot(tokens, query_weight, preferred_element_type=jnp.float32).reshape(row_count, head_count, head_size)
    keys_raw = jnp.dot(tokens, key_weight, preferred_element_type=jnp.float32).reshape(row_count, head_count, head_size)
    keys_raw = keys_raw * head_size ** (-0.5)
    values = jnp.dot(tokens, value_weight, preferred_element_type=jnp.float32).reshape(row_count, head_count, head_size)
    gating = jnp.dot(tokens, gate_weight, preferred_element_type=jnp.float32)
    query_rot = rotate(queries, lengths)
    key_rot = rotate(keys_raw, lengths)
    head_ids = jnp.arange(head_count, dtype=jnp.float32)
    decays = 1.0 - jnp.exp2(-2.0 - 10.0 * head_ids / (HEADS - 1))
    new_state = decays[None, :, None, None] * old_state + key_rot[:, :, :, None] * values[:, :, None, :]
    readout = jnp.einsum('thi,thij->thj', query_rot, new_state, precision=lax.Precision.HIGHEST)
    normed = layer_norm(readout, head_gain.reshape(head_count, head_size))
    mixed = (normed.reshape(row_count, head_count * head_size) * jax.nn.silu(gating)).astype(jnp.bfloat16)
    group_width = head_count * head_size // N_TP
    branch = jnp.zeros((row_count, model_width), jnp.float32)
    for shard_index in range(N_TP):
        lower = shard_index * group_width
        product = jnp.dot(mixed[:, lower:lower + group_width], output_weight[lower:lower + group_width], preferred_element_type=jnp.float32).astype(jnp.bfloat16)
        branch = branch + lax.optimization_barrier(product).astype(jnp.float32)
    after_mixer = layer_norm(RESIDUAL_SCALE * tokens.astype(jnp.float32) + branch, first_gain).astype(jnp.bfloat16)
    top_count = expert_ids.shape[1]
    expert_count = expert_gate.shape[0]
    slot_total = N_EP * CAP
    flat_ids = expert_ids.reshape(-1).astype(jnp.int32)
    pair_count = flat_ids.shape[0]
    onehot = (flat_ids[:, None] == jnp.arange(expert_count, dtype=jnp.int32)[None, :]).astype(jnp.int32)
    slot_rank = lax.optimization_barrier(jnp.sum(onehot * (jnp.cumsum(onehot, axis=0) - 1), axis=1))
    targets = (flat_ids * slot_total + slot_rank).astype(jnp.int32)
    owners = (jnp.arange(pair_count, dtype=jnp.int32) // top_count).astype(jnp.int32)
    table = jnp.zeros((expert_count * slot_total,), jnp.int32).at[targets].set(owners)
    gathered = after_mixer[table].reshape(expert_count, slot_total, model_width)
    hidden_width = expert_gate.shape[2] // N_TP

    def one_expert(operands):
        rows_in, gate_mat, up_mat, down_mat = operands
        gate_part = jnp.dot(rows_in, gate_mat, preferred_element_type=jnp.float32)
        up_part = jnp.dot(rows_in, up_mat, preferred_element_type=jnp.float32)
        hidden = (jax.nn.silu(gate_part) * up_part).astype(jnp.bfloat16)
        summed = jnp.zeros((rows_in.shape[0], model_width), jnp.float32)
        for shard_index in range(N_TP):
            lower = shard_index * hidden_width
            product = jnp.dot(hidden[:, lower:lower + hidden_width], down_mat[lower:lower + hidden_width], preferred_element_type=jnp.float32).astype(jnp.bfloat16)
            summed = summed + lax.optimization_barrier(product).astype(jnp.float32)
        return summed.astype(jnp.bfloat16)
    outputs = lax.map(one_expert, (gathered, expert_gate, expert_up, expert_down))
    picked = outputs.reshape(expert_count * slot_total, model_width)[targets].astype(jnp.float32)
    picked = picked.reshape(row_count, top_count, model_width)
    routed = lax.optimization_barrier(jnp.sum(picked * expert_weights[:, :, None], axis=1))
    switch = jax.nn.sigmoid(jnp.dot(after_mixer, side_gate, preferred_element_type=jnp.float32))
    dense_hidden = (jax.nn.silu(jnp.dot(after_mixer, dense_gate, preferred_element_type=jnp.float32)) * jnp.dot(after_mixer, dense_up, preferred_element_type=jnp.float32) * switch[:, None]).astype(jnp.bfloat16)
    shared_hidden = (jax.nn.silu(jnp.dot(after_mixer, shared_gate, preferred_element_type=jnp.float32)) * jnp.dot(after_mixer, shared_up, preferred_element_type=jnp.float32)).astype(jnp.bfloat16)
    side = (jnp.dot(dense_hidden, dense_down, preferred_element_type=jnp.float32) + jnp.dot(shared_hidden, shared_down, preferred_element_type=jnp.float32)).astype(jnp.bfloat16)
    total = RESIDUAL_SCALE * after_mixer.astype(jnp.float32) + routed + side.astype(jnp.float32)
    layer_out = layer_norm(total, second_gain).astype(jnp.bfloat16)
    return (layer_out, new_state)
```

```python
import functools

import jax
import jax.numpy as jnp
from jax import lax
from jax.experimental import pallas as pl
from jax.experimental.pallas import tpu as pltpu
from jax.sharding import PartitionSpec as P

MESH = pl.DeviceIdType.MESH
NORM_EPS = 1e-05
RESIDUAL_SCALE = 2.0**0.5
F32 = jnp.float32
BF16 = jnp.bfloat16
LANES = 128


def dot(left, right):
    return jnp.dot(left, right, preferred_element_type=F32)


def silu(x):
    return x * jax.nn.sigmoid(x)


def normalize(x, gain):
    centered = x - jnp.mean(x, axis=-1, keepdims=True)
    variance = jnp.mean(centered * centered, axis=-1, keepdims=True)
    return centered * lax.rsqrt(variance + NORM_EPS) * gain


def mixer_kernel(
    n_tp, tokens, turn_same, turn_other, head_gain, state_hbm, q_hbm, k_hbm, v_hbm, g_hbm, o_hbm,
    share_out, state_out, qw, kw, vw, gw, ow, state, fresh, readout, in_sem, state_sem, out_sem,
):
    rows, heads, size = state.shape[0], state.shape[1], state.shape[2]
    parts = state_sem.shape[0]
    span = rows // parts
    loads = []
    for at, (src, dst) in enumerate(((q_hbm, qw), (k_hbm, kw), (v_hbm, vw))):
        loads.append(pltpu.make_async_copy(src, dst, in_sem.at[at]))
    states = [
        pltpu.make_async_copy(
            state_hbm.at[pl.ds(p * span, span)], state.at[pl.ds(p * span, span)], state_sem.at[p]
        )
        for p in range(parts)
    ]
    late = [
        pltpu.make_async_copy(g_hbm, gw, in_sem.at[3]),
        pltpu.make_async_copy(o_hbm, ow, in_sem.at[4]),
    ]
    for copy in loads + states + late:
        copy.start()
    toks = tokens[...]
    loads[0].wait()
    queries = dot(toks, qw[...])
    loads[1].wait()
    keys = dot(toks, kw[...]) * size**-0.5
    same, other = turn_same[...], turn_other[...]

    def turned(x):
        return x * same + pltpu.roll(x, size // 2, 1) * other

    stack = []
    for h in range(heads):
        stack.append(turned(queries[:, h * size : (h + 1) * size]))
        stack.append(turned(keys[:, h * size : (h + 1) * size]))
    fill = size - 2 * heads * rows
    if fill:
        stack.append(jnp.zeros((fill, size), F32))
    columns = jnp.concatenate(stack, axis=0).T
    loads[2].wait()
    values = dot(toks, vw[...])
    first_head = lax.axis_index("tp") * heads
    decays = []
    for h in range(heads):
        number = (jnp.zeros((1, size), jnp.int32) + (first_head + h)).astype(F32)
        decays.append(1.0 - jnp.exp2(-2.0 - 10.0 * number / (heads * n_tp - 1)))
    writes = []
    for p in range(parts):
        states[p].wait()
        for t in range(p * span, (p + 1) * span):
            for h in range(heads):
                at = 2 * h * rows + t
                new = decays[h] * state[t, h] + columns[:, at + rows : at + rows + 1] * values[
                    t : t + 1, h * size : (h + 1) * size
                ]
                fresh[t, h] = new
                readout[t : t + 1, h * size : (h + 1) * size] = jnp.sum(
                    columns[:, at : at + 1] * new, axis=0, keepdims=True
                )
        write = pltpu.make_async_copy(
            fresh.at[pl.ds(p * span, span)], state_out.at[pl.ds(p * span, span)], out_sem.at[p]
        )
        write.start()
        writes.append(write)
    late[0].wait()
    gating = dot(toks, gw[...])
    late[1].wait()
    total = None
    for h in range(heads):
        cols = slice(h * size, (h + 1) * size)
        mixed = (normalize(readout[:, cols], head_gain[:, cols]) * silu(gating[:, cols])).astype(BF16)
        term = dot(mixed, ow[cols, :])
        total = term if total is None else total + term
    share_out[...] = total.astype(BF16)
    for write in writes:
        write.wait()


def layer_kernel(
    n_ep, n_tp,
    share, tokens, ids, id_weights, first_gain, second_gain, side_gate,
    dg_h, du_h, dd_h, eg_h, eu_h, ed_h, sg_h, su_h, sd_h,
    out,
    dg, du, dd, eg, eu, ed, sg, su, sd,
    got1, gathered, normed, switches, routing, hid_d, hid_e, hid_s, own_sum, core_out, core_in,
    y_out, y_in, total_out, ep_in, final,
    w_sem, s1, r1, sr, rr, sa, ra, sy, ry, sc, rc, s3, r3, s4, r4, s5, r5, s6, r6,
):
    ep, tp = lax.axis_index("ep"), lax.axis_index("tp")
    rows, width = tokens.shape
    cw = width // n_tp
    n_y = n_tp // 2
    y, core = tp // 2, lax.rem(tp, 2)
    mate = y * 2 + 1 - core
    barrier = pltpu.get_barrier_semaphore()

    def greet_ep(d, _):
        pl.semaphore_signal(
            barrier, inc=1, device_id=(lax.rem(ep + d, n_ep), tp), device_id_type=MESH
        )
        return 0

    def greet_tp(d, _):
        pl.semaphore_signal(
            barrier, inc=1, device_id=(ep, lax.rem(tp + d, n_tp)), device_id_type=MESH
        )
        return 0

    lax.fori_loop(1, n_ep, greet_ep, 0)
    lax.fori_loop(1, n_tp, greet_tp, 0)
    weights = [
        pltpu.make_async_copy(src, dst, w_sem.at[at])
        for at, (src, dst) in enumerate(
            ((dg_h, dg), (du_h, du), (eg_h, eg), (eu_h, eu), (sg_h, sg), (su_h, su), (dd_h, dd), (ed_h, ed), (sd_h, sd))
        )
    ]
    for copy in weights:
        copy.start()

    def rows_of(i):
        return pl.ds(pl.multiple_of(i * rows, rows), rows)

    def cols_of(j):
        return pl.ds(pl.multiple_of(j * cw, cw), cw)

    lane = lax.broadcasted_iota(jnp.int32, (rows, LANES), 1)
    mine = jnp.zeros((rows, LANES), F32)
    for k in range(ids.shape[1]):
        mine = mine + jnp.where(ids[:, k : k + 1] == lane, id_weights[:, k : k + 1], 0.0)
    routing[rows_of(ep), :] = mine
    hid_s[...] = jnp.zeros_like(hid_s)
    pl.semaphore_wait(barrier, n_ep + n_tp - 2)

    def copy1(d):
        peer = lax.rem(tp + d, n_tp)
        return pltpu.make_async_remote_copy(
            src_ref=share.at[:, cols_of(peer)], dst_ref=got1.at[d], send_sem=s1.at[d], recv_sem=r1.at[d],
            device_id=(ep, peer), device_id_type=MESH,
        )

    def copy_routing(d):
        return pltpu.make_async_remote_copy(
            src_ref=routing.at[rows_of(ep)], dst_ref=routing.at[rows_of(ep)], send_sem=sr.at[d],
            recv_sem=rr.at[d], device_id=(lax.rem(ep + d, n_ep), tp), device_id_type=MESH,
        )

    def routing_from(d):
        origin = rows_of(lax.rem(ep - d + n_ep, n_ep))
        return pltpu.make_async_remote_copy(
            src_ref=routing.at[origin], dst_ref=routing.at[origin], send_sem=sr.at[d],
            recv_sem=rr.at[d], device_id=(lax.rem(ep + d, n_ep), tp), device_id_type=MESH,
        )

    def loop(low, high, action):
        def step(d, carry):
            action(d)
            return carry

        lax.fori_loop(low, high, step, 0)

    loop(1, n_tp, lambda d: copy1(d).start())
    loop(1, n_ep, lambda d: copy_routing(d).start())
    piece = RESIDUAL_SCALE * tokens[:, cols_of(tp)].astype(F32) + share[:, cols_of(tp)].astype(F32)
    for d in range(1, n_tp):
        copy1(d).wait_recv()
        piece = piece + got1[d].astype(F32)
    gathered[rows_of(ep), cols_of(tp)] = piece.astype(BF16)

    def block(i, j):
        return gathered.at[rows_of(i), cols_of(j)]

    def ag(d, origin):
        return pltpu.make_async_remote_copy(
            src_ref=block(origin, tp), dst_ref=block(origin, tp), send_sem=sa.at[d], recv_sem=ra.at[d],
            device_id=(lax.rem(ep + d, n_ep), tp), device_id_type=MESH,
        )

    def along_y(d, e, j):
        peer = lax.rem(y + e, n_y) * 2 + core
        origin = lax.rem(ep - d + n_ep, n_ep)
        return pltpu.make_async_remote_copy(
            src_ref=block(origin, j), dst_ref=block(origin, j), send_sem=sy.at[e - 1, d],
            recv_sem=ry.at[e - 1, d], device_id=(ep, peer), device_id_type=MESH,
        )

    def to_mate(d, e, side):
        origin = lax.rem(ep - d + n_ep, n_ep)
        j = lax.rem(y - e + n_y, n_y) * 2 + side
        return pltpu.make_async_remote_copy(
            src_ref=block(origin, j), dst_ref=block(origin, j), send_sem=sc.at[e, d],
            recv_sem=rc.at[e, d], device_id=(ep, mate), device_id_type=MESH,
        )

    loop(1, n_ep, lambda d: ag(d, ep).start())

    def pass_on(d):
        for e in range(1, n_y):
            along_y(d, e, tp).start()
        to_mate(d, 0, core).start()

    pass_on(0)

    def arrived(d):
        ag(d, lax.rem(ep - d + n_ep, n_ep)).wait_recv()
        pass_on(d)

    loop(1, n_ep, arrived)

    def over(d):
        for e in range(1, n_y):
            along_y(d, e, lax.rem(y - e + n_y, n_y) * 2 + core).wait_recv()
            to_mate(d, e, core).start()

    loop(0, n_ep, over)

    gain1 = first_gain[...]
    side = side_gate[...].astype(F32)

    def finish(d):
        for e in range(n_y):
            to_mate(d, e, 1 - core).wait_recv()
        where = rows_of(lax.rem(ep - d + n_ep, n_ep))
        after = normalize(gathered[where, :].astype(F32), gain1).astype(BF16)
        normed[where, :] = after
        turned = jax.nn.sigmoid(jnp.sum(after.astype(F32) * side, axis=-1, keepdims=True))
        switches[where, :] = jnp.broadcast_to(turned, (rows, LANES))

    loop(0, n_ep, finish)
    loop(1, n_ep, lambda d: routing_from(d).wait_recv())

    everyone = normed[...]
    weights[0].wait()
    gate = dot(everyone, dg[...])
    weights[1].wait()
    up = dot(everyone, du[...])
    hid_d[...] = (silu(gate) * up * switches[:, 0:1]).astype(BF16)
    weights[2].wait()
    weights[3].wait()
    experts = eg.shape[0]
    lanes = lax.broadcasted_iota(jnp.int32, routing.shape, 1)
    for e in range(experts):
        weight = jnp.sum(
            jnp.where(lanes == ep * experts + e, routing[...], 0.0), axis=-1, keepdims=True
        )
        hid_e[e] = (silu(dot(everyone, eg[e])) * dot(everyone, eu[e]) * weight).astype(BF16)
    weights[4].wait()
    weights[5].wait()
    own = normed[rows_of(ep), :]
    hid_s[rows_of(ep), :] = (silu(dot(own, sg[...])) * dot(own, su[...])).astype(BF16)
    for at in (6, 7, 8):
        weights[at].wait()

    def product(j):
        cols = cols_of(j)
        result = dot(hid_d[...], dd[:, cols]) + dot(hid_s[...], sd[:, cols])
        for e in range(experts):
            result = result + dot(hid_e[e], ed[e, :, cols])
        return result

    def core_copy(e):
        return pltpu.make_async_remote_copy(
            src_ref=core_out.at[e], dst_ref=core_in.at[e], send_sem=s3.at[e], recv_sem=r3.at[e],
            device_id=(ep, mate), device_id_type=MESH,
        )

    def y_copy(e):
        peer = lax.rem(y + e, n_y) * 2 + core
        return pltpu.make_async_remote_copy(
            src_ref=y_out.at[e - 1], dst_ref=y_in.at[e - 1], send_sem=s4.at[e - 1], recv_sem=r4.at[e - 1],
            device_id=(ep, peer), device_id_type=MESH,
        )

    for e in list(range(1, n_y)) + [0]:
        target = lax.rem(y + e, n_y) * 2
        core_out[e] = product(target + 1 - core).astype(BF16)
        core_copy(e).start()
        own_sum[...] = product(target + core)
        core_copy(e).wait_recv()
        if e:
            y_out[e - 1] = (own_sum[...] + core_in[e].astype(F32)).astype(BF16)
            y_copy(e).start()
    total = own_sum[...] + core_in[0].astype(F32)
    for e in range(1, n_y):
        y_copy(e).wait_recv()
        total = total + y_in[e - 1].astype(F32)
    total_out[...] = total.astype(BF16)

    def ep_copy(d):
        peer = lax.rem(ep + d, n_ep)
        return pltpu.make_async_remote_copy(
            src_ref=total_out.at[rows_of(peer)], dst_ref=ep_in.at[d], send_sem=s5.at[d],
            recv_sem=r5.at[d], device_id=(peer, tp), device_id_type=MESH,
        )

    loop(1, n_ep, lambda d: ep_copy(d).start())

    def gather_sum(d, so_far):
        ep_copy(d).wait_recv()
        return so_far + ep_in[d].astype(F32)

    mine = lax.fori_loop(1, n_ep, gather_sum, total_out[rows_of(ep), :].astype(F32))
    final[:, cols_of(tp)] = mine.astype(BF16)

    def last_copy(d, j):
        return pltpu.make_async_remote_copy(
            src_ref=final.at[:, cols_of(j)], dst_ref=final.at[:, cols_of(j)], send_sem=s6.at[d],
            recv_sem=r6.at[d], device_id=(ep, lax.rem(tp + d, n_tp)), device_id_type=MESH,
        )

    loop(1, n_tp, lambda d: last_copy(d, tp).start())
    loop(1, n_tp, lambda d: last_copy(d, lax.rem(tp - d + n_tp, n_tp)).wait_recv())
    result = RESIDUAL_SCALE * normed[rows_of(ep), :].astype(F32) + final[...].astype(F32)
    out[...] = normalize(result, second_gain[...]).astype(BF16)

    def settle(d):
        ag(d, ep).wait_send()
        copy_routing(d).wait_send()
        ep_copy(d).wait_send()

    loop(1, n_ep, settle)

    def settle_tp(d):
        copy1(d).wait_send()
        last_copy(d, tp).wait_send()

    loop(1, n_tp, settle_tp)

    def settle_forward(d):
        for e in range(n_y):
            to_mate(d, e, core).wait_send()
            if e:
                along_y(d, e, tp).wait_send()

    loop(0, n_ep, settle_forward)
    for e in range(n_y):
        core_copy(e).wait_send()
        if e:
            y_copy(e).wait_send()


def per_device(
    n_ep, n_tp,
    tokens, lengths, old_state, query_weight, key_weight, value_weight, gate_weight, head_gain,
    output_weight, first_gain, expert_ids, expert_weights, expert_gate, expert_up, expert_down,
    shared_gate, shared_up, shared_down, side_gate, dense_gate, dense_up, dense_down, second_gain,
):
    rows, width = tokens.shape
    heads, size = old_state.shape[1], old_state.shape[-1]
    half = size // 2
    frequency = 1.0 / 10000.0 ** (jnp.arange(half, dtype=F32) * 2.0 / size)
    angles = lengths.astype(F32)[:, None] * frequency[None, :]
    cosine, sine = jnp.cos(angles), jnp.sin(angles)
    turn_same = jnp.concatenate([cosine, cosine], axis=1)
    turn_other = jnp.concatenate([-sine, sine], axis=1)
    inner = heads * size
    vmem = pl.BlockSpec(memory_space=pltpu.VMEM)
    anywhere = pl.BlockSpec(memory_space=pl.ANY)
    parts = 4
    dma = pltpu.SemaphoreType.DMA
    share, new_state = pl.pallas_call(
        functools.partial(mixer_kernel, n_tp),
        out_shape=(
            jax.ShapeDtypeStruct((rows, width), BF16),
            jax.ShapeDtypeStruct(old_state.shape, F32),
        ),
        in_specs=[vmem] * 4 + [anywhere] * 6,
        out_specs=(vmem, anywhere),
        scratch_shapes=[pltpu.VMEM((width, inner), BF16)] * 4
        + [
            pltpu.VMEM((inner, width), BF16),
            pltpu.VMEM(old_state.shape, F32),
            pltpu.VMEM(old_state.shape, F32),
            pltpu.VMEM((rows, inner), F32),
            dma((5,)),
            dma((parts,)),
            dma((parts,)),
        ],
        name="mixer",
    )(
        tokens, turn_same, turn_other, head_gain.reshape(1, -1), old_state, query_weight, key_weight,
        value_weight, gate_weight, output_weight,
    )
    cw = width // n_tp
    n_y = n_tp // 2
    everyone = rows * n_ep
    big = [dense_gate, dense_up, dense_down, expert_gate, expert_up, expert_down, shared_gate, shared_up, shared_down]
    layer_out = pl.pallas_call(
        functools.partial(layer_kernel, n_ep, n_tp),
        out_shape=jax.ShapeDtypeStruct((rows, width), BF16),
        in_specs=[vmem] * 7 + [anywhere] * len(big),
        out_specs=vmem,
        scratch_shapes=[pltpu.VMEM(w.shape, BF16) for w in big]
        + [
            pltpu.VMEM((n_tp, rows, cw), BF16),
            pltpu.VMEM((everyone, width), BF16),
            pltpu.VMEM((everyone, width), BF16),
            pltpu.VMEM((everyone, LANES), F32),
            pltpu.VMEM((everyone, LANES), F32),
            pltpu.VMEM((everyone, dense_gate.shape[1]), BF16),
            pltpu.VMEM((expert_gate.shape[0], everyone, expert_gate.shape[2]), BF16),
            pltpu.VMEM((everyone, shared_gate.shape[1]), BF16),
            pltpu.VMEM((everyone, cw), F32),
            pltpu.VMEM((n_y, everyone, cw), BF16),
            pltpu.VMEM((n_y, everyone, cw), BF16),
            pltpu.VMEM((n_y - 1, everyone, cw), BF16),
            pltpu.VMEM((n_y - 1, everyone, cw), BF16),
            pltpu.VMEM((everyone, cw), BF16),
            pltpu.VMEM((n_ep, rows, cw), BF16),
            pltpu.VMEM((rows, width), BF16),
            dma((len(big),)),
        ]
        + [dma((n_tp,))] * 2
        + [dma((n_ep,))] * 4
        + [dma((n_y - 1, n_ep))] * 2
        + [dma((n_y, n_ep))] * 2
        + [dma((n_y,))] * 2
        + [dma((n_y - 1,))] * 2
        + [dma((n_ep,))] * 2
        + [dma((n_tp,))] * 2,
        compiler_params=pltpu.CompilerParams(collective_id=0, has_side_effects=True),
        name="layer",
    )(
        share, tokens, expert_ids, expert_weights, first_gain.reshape(1, -1),
        second_gain.reshape(1, -1), side_gate.reshape(1, -1), *big,
    )
    return layer_out, new_state


def solution(mesh):
    return jax.shard_map(
        functools.partial(per_device, mesh.shape["ep"], mesh.shape["tp"]),
        mesh=mesh,
        in_specs=(
            P("ep", None),
            P("ep"),
            P("ep", "tp", None, None),
            P(None, "tp"),
            P(None, "tp"),
            P(None, "tp"),
            P(None, "tp"),
            P("tp"),
            P("tp", None),
            P(),
            P("ep", None),
            P("ep", None),
            P("ep", None, "tp"),
            P("ep", None, "tp"),
            P("ep", "tp", None),
            P(None, "tp"),
            P(None, "tp"),
            P("tp", None),
            P(),
            P(None, ("ep", "tp")),
            P(None, ("ep", "tp")),
            P(("ep", "tp"), None),
            P(),
        ),
        out_specs=(P("ep", None), P("ep", "tp", None, None)),
        check_vma=False,
    )
```

```python
import functools

import jax
import jax.numpy as jnp
import numpy as np
from jax import lax
from jax.experimental import pallas as pl
from jax.experimental.pallas import tpu as pltpu
from jax.sharding import PartitionSpec as P

MESH = pl.DeviceIdType.MESH
NORM_EPS = 1e-05
RESIDUAL_SCALE = 2.0**0.5
F32 = jnp.float32
BF16 = jnp.bfloat16
LANES = 128


def dot(left, right):
    return jnp.dot(left, right, preferred_element_type=F32)


def silu(x):
    return x * jax.nn.sigmoid(x)


def normalize(x, gain):
    centered = x - jnp.mean(x, axis=-1, keepdims=True)
    variance = jnp.mean(centered * centered, axis=-1, keepdims=True)
    return centered * lax.rsqrt(variance + NORM_EPS) * gain


def mixer_kernel(
    n_tp, lengths, tokens, frequency, head_gain, state_hbm, q_hbm, k_hbm, v_hbm, g_hbm, o_hbm,
    share_out, state_out, qw, kw, vw, gw, ow, state, fresh, readout, in_sem, state_sem, out_sem,
):
    rows, heads, size = state.shape[0], state.shape[1], state.shape[2]
    parts = state_sem.shape[0]
    span = rows // parts
    loads = []
    for at, (src, dst) in enumerate(((q_hbm, qw), (k_hbm, kw), (v_hbm, vw))):
        loads.append(pltpu.make_async_copy(src, dst, in_sem.at[at]))
    states = [
        pltpu.make_async_copy(
            state_hbm.at[pl.ds(p * span, span)], state.at[pl.ds(p * span, span)], state_sem.at[p]
        )
        for p in range(parts)
    ]
    late = [
        pltpu.make_async_copy(g_hbm, gw, in_sem.at[3]),
        pltpu.make_async_copy(o_hbm, ow, in_sem.at[4]),
    ]
    for copy in loads + states + late:
        copy.start()
    toks = tokens[...]
    positions = jnp.concatenate(
        [jnp.zeros((1, size), jnp.int32) + lengths[t] for t in range(rows)], axis=0
    ).astype(F32)
    angles = positions * frequency[...]
    turns = jnp.floor(angles * (0.5 / np.pi) + 0.5)
    angles = (angles - turns * 6.28125) - turns * (2.0 * np.pi - 6.28125)
    sine = jnp.sin(angles)
    first = lax.broadcasted_iota(jnp.int32, (rows, size), 1) < size // 2
    same, other = jnp.cos(angles), jnp.where(first, -sine, sine)
    loads[0].wait()
    queries = dot(toks, qw[...])
    loads[1].wait()
    keys = dot(toks, kw[...]) * size**-0.5

    def turned(x):
        return x * same + pltpu.roll(x, size // 2, 1) * other

    stack = []
    for h in range(heads):
        stack.append(turned(queries[:, h * size : (h + 1) * size]))
        stack.append(turned(keys[:, h * size : (h + 1) * size]))
    fill = size - 2 * heads * rows
    if fill:
        stack.append(jnp.zeros((fill, size), F32))
    columns = jnp.concatenate(stack, axis=0).T
    loads[2].wait()
    values = dot(toks, vw[...])
    first_head = lax.axis_index("tp") * heads
    decays = []
    for h in range(heads):
        number = (jnp.zeros((1, size), jnp.int32) + (first_head + h)).astype(F32)
        decays.append(1.0 - jnp.exp2(-2.0 - 10.0 * number / (heads * n_tp - 1)))
    writes = []
    for p in range(parts):
        states[p].wait()
        for t in range(p * span, (p + 1) * span):
            for h in range(heads):
                at = 2 * h * rows + t
                new = decays[h] * state[t, h] + columns[:, at + rows : at + rows + 1] * values[
                    t : t + 1, h * size : (h + 1) * size
                ]
                fresh[t, h] = new
                readout[t : t + 1, h * size : (h + 1) * size] = jnp.sum(
                    columns[:, at : at + 1] * new, axis=0, keepdims=True
                )
        write = pltpu.make_async_copy(
            fresh.at[pl.ds(p * span, span)], state_out.at[pl.ds(p * span, span)], out_sem.at[p]
        )
        write.start()
        writes.append(write)
    late[0].wait()
    gating = dot(toks, gw[...])
    late[1].wait()
    total = None
    for h in range(heads):
        cols = slice(h * size, (h + 1) * size)
        mixed = (normalize(readout[:, cols], head_gain[:, cols]) * silu(gating[:, cols])).astype(BF16)
        term = dot(mixed, ow[cols, :])
        total = term if total is None else total + term
    share_out[...] = total.astype(BF16)
    for write in writes:
        write.wait()


def layer_kernel(
    n_ep, n_tp,
    share, tokens, ids, id_weights, first_gain, second_gain, side_gate,
    dg_h, du_h, dd_h, eg_h, eu_h, ed_h, sg_h, su_h, sd_h,
    out,
    dg, du, dd, eg, eu, ed, sg, su, sd,
    got1, gathered, normed, switches, routing, hid_d, hid_e, hid_s, own_sum, core_out, core_in,
    y_out, y_in, total_out, ep_in, final,
    w_sem, s1, r1, sr, rr, sa, ra, sy, ry, sc, rc, s3, r3, s4, r4, s5, r5, s6, r6,
):
    ep, tp = lax.axis_index("ep"), lax.axis_index("tp")
    rows, width = tokens.shape
    cw = width // n_tp
    n_y = n_tp // 2
    y, core = tp // 2, lax.rem(tp, 2)
    mate = y * 2 + 1 - core
    barrier = pltpu.get_barrier_semaphore()

    def greet_ep(d, _):
        pl.semaphore_signal(
            barrier, inc=1, device_id=(lax.rem(ep + d, n_ep), tp), device_id_type=MESH
        )
        return 0

    def greet_tp(d, _):
        pl.semaphore_signal(
            barrier, inc=1, device_id=(ep, lax.rem(tp + d, n_tp)), device_id_type=MESH
        )
        return 0

    lax.fori_loop(1, n_ep, greet_ep, 0)
    lax.fori_loop(1, n_tp, greet_tp, 0)
    weights = [
        pltpu.make_async_copy(src, dst, w_sem.at[at])
        for at, (src, dst) in enumerate(
            ((dg_h, dg), (du_h, du), (eg_h, eg), (eu_h, eu), (sg_h, sg), (su_h, su), (dd_h, dd), (ed_h, ed), (sd_h, sd))
        )
    ]
    for copy in weights:
        copy.start()

    def rows_of(i):
        return pl.ds(pl.multiple_of(i * rows, rows), rows)

    def cols_of(j):
        return pl.ds(pl.multiple_of(j * cw, cw), cw)

    number = lax.broadcasted_iota(jnp.int32, (LANES, rows), 0)
    columns = jnp.zeros((LANES, rows), F32)
    for k in range(ids.shape[0]):
        columns = columns + jnp.where(ids[k : k + 1, :] == number, id_weights[k : k + 1, :], 0.0)
    unit = (
        lax.broadcasted_iota(jnp.int32, (rows, rows), 0) == lax.broadcasted_iota(jnp.int32, (rows, rows), 1)
    ).astype(F32)
    mine = lax.dot_general(
        unit, columns, (((1,), (1,)), ((), ())), precision=lax.Precision.HIGHEST, preferred_element_type=F32
    )
    routing[rows_of(ep), :] = mine
    hid_s[...] = jnp.zeros_like(hid_s)
    pl.semaphore_wait(barrier, n_ep + n_tp - 2)

    def copy1(d):
        peer = lax.rem(tp + d, n_tp)
        return pltpu.make_async_remote_copy(
            src_ref=share.at[:, cols_of(peer)], dst_ref=got1.at[d], send_sem=s1.at[d], recv_sem=r1.at[d],
            device_id=(ep, peer), device_id_type=MESH,
        )

    def copy_routing(d):
        return pltpu.make_async_remote_copy(
            src_ref=routing.at[rows_of(ep)], dst_ref=routing.at[rows_of(ep)], send_sem=sr.at[d],
            recv_sem=rr.at[d], device_id=(lax.rem(ep + d, n_ep), tp), device_id_type=MESH,
        )

    def routing_from(d):
        origin = rows_of(lax.rem(ep - d + n_ep, n_ep))
        return pltpu.make_async_remote_copy(
            src_ref=routing.at[origin], dst_ref=routing.at[origin], send_sem=sr.at[d],
            recv_sem=rr.at[d], device_id=(lax.rem(ep + d, n_ep), tp), device_id_type=MESH,
        )

    def loop(low, high, action):
        def step(d, carry):
            action(d)
            return carry

        lax.fori_loop(low, high, step, 0)

    loop(1, n_tp, lambda d: copy1(d).start())
    loop(1, n_ep, lambda d: copy_routing(d).start())
    piece = RESIDUAL_SCALE * tokens[:, cols_of(tp)].astype(F32) + share[:, cols_of(tp)].astype(F32)
    for d in range(1, n_tp):
        copy1(d).wait_recv()
        piece = piece + got1[d].astype(F32)
    gathered[rows_of(ep), cols_of(tp)] = piece.astype(BF16)

    def block(i, j):
        return gathered.at[rows_of(i), cols_of(j)]

    def ag(d, origin):
        return pltpu.make_async_remote_copy(
            src_ref=block(origin, tp), dst_ref=block(origin, tp), send_sem=sa.at[d], recv_sem=ra.at[d],
            device_id=(lax.rem(ep + d, n_ep), tp), device_id_type=MESH,
        )

    def along_y(d, e, j):
        peer = lax.rem(y + e, n_y) * 2 + core
        origin = lax.rem(ep - d + n_ep, n_ep)
        return pltpu.make_async_remote_copy(
            src_ref=block(origin, j), dst_ref=block(origin, j), send_sem=sy.at[e - 1, d],
            recv_sem=ry.at[e - 1, d], device_id=(ep, peer), device_id_type=MESH,
        )

    def to_mate(d, e, side):
        origin = lax.rem(ep - d + n_ep, n_ep)
        j = lax.rem(y - e + n_y, n_y) * 2 + side
        return pltpu.make_async_remote_copy(
            src_ref=block(origin, j), dst_ref=block(origin, j), send_sem=sc.at[e, d],
            recv_sem=rc.at[e, d], device_id=(ep, mate), device_id_type=MESH,
        )

    loop(1, n_ep, lambda d: ag(d, ep).start())

    def pass_on(d):
        for e in range(1, n_y):
            along_y(d, e, tp).start()
        to_mate(d, 0, core).start()

    pass_on(0)

    def arrived(d):
        ag(d, lax.rem(ep - d + n_ep, n_ep)).wait_recv()
        pass_on(d)

    loop(1, n_ep, arrived)

    def over(d):
        for e in range(1, n_y):
            along_y(d, e, lax.rem(y - e + n_y, n_y) * 2 + core).wait_recv()
            to_mate(d, e, core).start()

    loop(0, n_ep, over)

    gain1 = first_gain[...]
    side = side_gate[...].astype(F32)
    side = jnp.concatenate([side[r : r + 1, :] for r in range(width // LANES)], axis=1)

    def finish(d):
        for e in range(n_y):
            to_mate(d, e, 1 - core).wait_recv()
        where = rows_of(lax.rem(ep - d + n_ep, n_ep))
        after = normalize(gathered[where, :].astype(F32), gain1).astype(BF16)
        normed[where, :] = after
        turned = jax.nn.sigmoid(jnp.sum(after.astype(F32) * side, axis=-1, keepdims=True))
        switches[where, :] = jnp.broadcast_to(turned, (rows, LANES))

    loop(0, n_ep, finish)
    loop(1, n_ep, lambda d: routing_from(d).wait_recv())

    everyone = normed[...]
    weights[0].wait()
    gate = dot(everyone, dg[...])
    weights[1].wait()
    up = dot(everyone, du[...])
    hid_d[...] = (silu(gate) * up * switches[:, 0:1]).astype(BF16)
    weights[2].wait()
    weights[3].wait()
    experts = eg.shape[0]
    lanes = lax.broadcasted_iota(jnp.int32, routing.shape, 1)
    for e in range(experts):
        weight = jnp.sum(
            jnp.where(lanes == ep * experts + e, routing[...], 0.0), axis=-1, keepdims=True
        )
        hid_e[e] = (silu(dot(everyone, eg[e])) * dot(everyone, eu[e]) * weight).astype(BF16)
    weights[4].wait()
    weights[5].wait()
    own = normed[rows_of(ep), :]
    hid_s[rows_of(ep), :] = (silu(dot(own, sg[...])) * dot(own, su[...])).astype(BF16)
    for at in (6, 7, 8):
        weights[at].wait()

    near_ep = n_ep // 2
    half_rows = near_ep * rows
    near = ep // near_ep

    def half_of(s):
        which = near if s else 1 - near
        return pl.ds(pl.multiple_of(which * half_rows, half_rows), half_rows)

    def product(s, j):
        where, cols = half_of(s), cols_of(j)
        result = dot(hid_d[where, :], dd[:, cols]) + dot(hid_s[where, :], sd[:, cols])
        for e in range(experts):
            result = result + dot(hid_e[e, where, :], ed[e, :, cols])
        return result

    def core_copy(s, e):
        at = s * n_y + e
        return pltpu.make_async_remote_copy(
            src_ref=core_out.at[at], dst_ref=core_in.at[at], send_sem=s3.at[at], recv_sem=r3.at[at],
            device_id=(ep, mate), device_id_type=MESH,
        )

    def y_copy(s, e):
        at = s * (n_y - 1) + e - 1
        peer = lax.rem(y + e, n_y) * 2 + core
        return pltpu.make_async_remote_copy(
            src_ref=y_out.at[at], dst_ref=y_in.at[at], send_sem=s4.at[at], recv_sem=r4.at[at],
            device_id=(ep, peer), device_id_type=MESH,
        )

    def ep_copy(d):
        peer = lax.rem(ep + d, n_ep)
        return pltpu.make_async_remote_copy(
            src_ref=total_out.at[rows_of(peer)], dst_ref=ep_in.at[d], send_sem=s5.at[d],
            recv_sem=r5.at[d], device_id=(peer, tp), device_id_type=MESH,
        )

    def terms(s, e):
        target = lax.rem(y + e, n_y) * 2
        at = s * n_y + e
        core_out[at] = product(s, target + 1 - core).astype(BF16)
        core_copy(s, e).start()
        own_sum[s] = product(s, target + core)
        if e:
            core_copy(s, e).wait_recv()
            y_out[s * (n_y - 1) + e - 1] = (own_sum[s] + core_in[at].astype(F32)).astype(BF16)
            y_copy(s, e).start()

    def send_total(s):
        core_copy(s, 0).wait_recv()
        total = own_sum[s] + core_in[s * n_y].astype(F32)
        for e in range(1, n_y):
            y_copy(s, e).wait_recv()
            total = total + y_in[s * (n_y - 1) + e - 1].astype(F32)
        total_out[half_of(s), :] = total.astype(BF16)
        if s:
            base = near * near_ep
            inside = ep - base
            loop(1, near_ep, lambda m: ep_copy(lax.rem(base + lax.rem(inside + m, near_ep) - ep + n_ep, n_ep)).start())
        else:
            base = (1 - near) * near_ep
            loop(0, near_ep, lambda m: ep_copy(lax.rem(base + m - ep + n_ep, n_ep)).start())

    for e in range(1, n_y):
        terms(0, e)
    terms(0, 0)
    for e in range(1, n_y):
        terms(1, e)
    send_total(0)
    terms(1, 0)
    send_total(1)

    def gather_sum(d, so_far):
        ep_copy(d).wait_recv()
        return so_far + ep_in[d].astype(F32)

    mine = lax.fori_loop(1, n_ep, gather_sum, total_out[rows_of(ep), :].astype(F32))
    final[:, cols_of(tp)] = mine.astype(BF16)

    def last_copy(d, j):
        return pltpu.make_async_remote_copy(
            src_ref=final.at[:, cols_of(j)], dst_ref=final.at[:, cols_of(j)], send_sem=s6.at[d],
            recv_sem=r6.at[d], device_id=(ep, lax.rem(tp + d, n_tp)), device_id_type=MESH,
        )

    loop(1, n_tp, lambda d: last_copy(d, tp).start())
    loop(1, n_tp, lambda d: last_copy(d, lax.rem(tp - d + n_tp, n_tp)).wait_recv())
    result = RESIDUAL_SCALE * normed[rows_of(ep), :].astype(F32) + final[...].astype(F32)
    out[...] = normalize(result, second_gain[...]).astype(BF16)

    def settle(d):
        ag(d, ep).wait_send()
        copy_routing(d).wait_send()
        ep_copy(d).wait_send()

    loop(1, n_ep, settle)

    def settle_tp(d):
        copy1(d).wait_send()
        last_copy(d, tp).wait_send()

    loop(1, n_tp, settle_tp)

    def settle_forward(d):
        for e in range(n_y):
            to_mate(d, e, core).wait_send()
            if e:
                along_y(d, e, tp).wait_send()

    loop(0, n_ep, settle_forward)
    for s in range(2):
        for e in range(n_y):
            core_copy(s, e).wait_send()
            if e:
                y_copy(s, e).wait_send()


def per_device(
    n_ep, n_tp,
    tokens, lengths, old_state, query_weight, key_weight, value_weight, gate_weight, head_gain,
    output_weight, first_gain, expert_ids, expert_weights, expert_gate, expert_up, expert_down,
    shared_gate, shared_up, shared_down, side_gate, dense_gate, dense_up, dense_down, second_gain,
):
    rows, width = tokens.shape
    heads, size = old_state.shape[1], old_state.shape[-1]
    half = size // 2
    frequency = np.tile(10000.0 ** (-np.arange(half) * 2.0 / size), 2)[None].astype(np.float32)
    inner = heads * size
    vmem = pl.BlockSpec(memory_space=pltpu.VMEM)
    anywhere = pl.BlockSpec(memory_space=pl.ANY)
    parts = 4
    dma = pltpu.SemaphoreType.DMA
    share, new_state = pl.pallas_call(
        functools.partial(mixer_kernel, n_tp),
        out_shape=(
            jax.ShapeDtypeStruct((rows, width), BF16),
            jax.ShapeDtypeStruct(old_state.shape, F32),
        ),
        in_specs=[pl.BlockSpec(memory_space=pltpu.SMEM)] + [vmem] * 3 + [anywhere] * 6,
        out_specs=(vmem, anywhere),
        scratch_shapes=[pltpu.VMEM((width, inner), BF16)] * 4
        + [
            pltpu.VMEM((inner, width), BF16),
            pltpu.VMEM(old_state.shape, F32),
            pltpu.VMEM(old_state.shape, F32),
            pltpu.VMEM((rows, inner), F32),
            dma((5,)),
            dma((parts,)),
            dma((parts,)),
        ],
        name="mixer",
    )(
        lengths, tokens, jnp.asarray(frequency), head_gain.reshape(1, -1), old_state, query_weight, key_weight,
        value_weight, gate_weight, output_weight,
    )
    cw = width // n_tp
    n_y = n_tp // 2
    everyone = rows * n_ep
    big = [dense_gate, dense_up, dense_down, expert_gate, expert_up, expert_down, shared_gate, shared_up, shared_down]
    layer_out = pl.pallas_call(
        functools.partial(layer_kernel, n_ep, n_tp),
        out_shape=jax.ShapeDtypeStruct((rows, width), BF16),
        in_specs=[vmem] * 7 + [anywhere] * len(big),
        out_specs=vmem,
        scratch_shapes=[pltpu.VMEM(w.shape, BF16) for w in big]
        + [
            pltpu.VMEM((n_tp, rows, cw), BF16),
            pltpu.VMEM((everyone, width), BF16),
            pltpu.VMEM((everyone, width), BF16),
            pltpu.VMEM((everyone, LANES), F32),
            pltpu.VMEM((everyone, LANES), F32),
            pltpu.VMEM((everyone, dense_gate.shape[1]), BF16),
            pltpu.VMEM((expert_gate.shape[0], everyone, expert_gate.shape[2]), BF16),
            pltpu.VMEM((everyone, shared_gate.shape[1]), BF16),
            pltpu.VMEM((2, everyone // 2, cw), F32),
            pltpu.VMEM((2 * n_y, everyone // 2, cw), BF16),
            pltpu.VMEM((2 * n_y, everyone // 2, cw), BF16),
            pltpu.VMEM((2 * (n_y - 1), everyone // 2, cw), BF16),
            pltpu.VMEM((2 * (n_y - 1), everyone // 2, cw), BF16),
            pltpu.VMEM((everyone, cw), BF16),
            pltpu.VMEM((n_ep, rows, cw), BF16),
            pltpu.VMEM((rows, width), BF16),
            dma((len(big),)),
        ]
        + [dma((n_tp,))] * 2
        + [dma((n_ep,))] * 4
        + [dma((n_y - 1, n_ep))] * 2
        + [dma((n_y, n_ep))] * 2
        + [dma((2 * n_y,))] * 2
        + [dma((2 * (n_y - 1),))] * 2
        + [dma((n_ep,))] * 2
        + [dma((n_tp,))] * 2,
        compiler_params=pltpu.CompilerParams(collective_id=0, has_side_effects=True),
        name="layer",
    )(
        share, tokens, expert_ids.T, expert_weights.T, first_gain.reshape(1, -1),
        second_gain.reshape(1, -1), side_gate.reshape(-1, LANES), *big,
    )
    return layer_out, new_state


def solution(mesh):
    return jax.shard_map(
        functools.partial(per_device, mesh.shape["ep"], mesh.shape["tp"]),
        mesh=mesh,
        in_specs=(
            P("ep", None),
            P("ep"),
            P("ep", "tp", None, None),
            P(None, "tp"),
            P(None, "tp"),
            P(None, "tp"),
            P(None, "tp"),
            P("tp"),
            P("tp", None),
            P(),
            P("ep", None),
            P("ep", None),
            P("ep", None, "tp"),
            P("ep", None, "tp"),
            P("ep", "tp", None),
            P(None, "tp"),
            P(None, "tp"),
            P("tp", None),
            P(),
            P(None, ("ep", "tp")),
            P(None, ("ep", "tp")),
            P(("ep", "tp"), None),
            P(),
        ),
        out_specs=(P("ep", None), P("ep", "tp", None, None)),
        check_vma=False,
    )
```

```python
import functools

import jax
import jax.numpy as jnp
import numpy as np
from jax import lax
from jax.experimental import pallas as pl
from jax.experimental.pallas import tpu as pltpu
from jax.sharding import PartitionSpec as P

MESH = pl.DeviceIdType.MESH
NORM_EPS = 1e-05
RESIDUAL_SCALE = 2.0**0.5
F32 = jnp.float32
BF16 = jnp.bfloat16
LANES = 128


def dot(left, right):
    return jnp.dot(left, right, preferred_element_type=F32)


def silu(x):
    return x * jax.nn.sigmoid(x)


def normalize(x, gain):
    centered = x - jnp.mean(x, axis=-1, keepdims=True)
    variance = jnp.mean(centered * centered, axis=-1, keepdims=True)
    return centered * lax.rsqrt(variance + NORM_EPS) * gain


def mixer_kernel(
    n_tp, lengths, tokens, frequency, head_gain, state_hbm, q_hbm, k_hbm, v_hbm, g_hbm, o_hbm,
    share_out, state_out, qw, kw, vw, gw, ow, state, fresh, readout, in_sem, state_sem, out_sem,
):
    rows, heads, size = state.shape[0], state.shape[1], state.shape[2]
    parts = state_sem.shape[0]
    span = rows // parts
    loads = []
    for at, (src, dst) in enumerate(((q_hbm, qw), (k_hbm, kw), (v_hbm, vw))):
        loads.append(pltpu.make_async_copy(src, dst, in_sem.at[at]))
    states = [
        pltpu.make_async_copy(
            state_hbm.at[pl.ds(p * span, span)], state.at[pl.ds(p * span, span)], state_sem.at[p]
        )
        for p in range(parts)
    ]
    late = [
        pltpu.make_async_copy(g_hbm, gw, in_sem.at[3]),
        pltpu.make_async_copy(o_hbm, ow, in_sem.at[4]),
    ]
    for copy in loads + states + late:
        copy.start()
    toks = tokens[...]
    positions = jnp.concatenate(
        [jnp.zeros((1, size), jnp.int32) + lengths[t] for t in range(rows)], axis=0
    ).astype(F32)
    angles = positions * frequency[...]
    turns = jnp.floor(angles * (0.5 / np.pi) + 0.5)
    angles = (angles - turns * 6.28125) - turns * (2.0 * np.pi - 6.28125)
    sine = jnp.sin(angles)
    first = lax.broadcasted_iota(jnp.int32, (rows, size), 1) < size // 2
    same, other = jnp.cos(angles), jnp.where(first, -sine, sine)
    loads[0].wait()
    queries = dot(toks, qw[...])
    loads[1].wait()
    keys = dot(toks, kw[...]) * size**-0.5

    def turned(x):
        return x * same + pltpu.roll(x, size // 2, 1) * other

    stack = []
    for h in range(heads):
        stack.append(turned(queries[:, h * size : (h + 1) * size]))
        stack.append(turned(keys[:, h * size : (h + 1) * size]))
    fill = size - 2 * heads * rows
    if fill:
        stack.append(jnp.zeros((fill, size), F32))
    columns = jnp.concatenate(stack, axis=0).T
    loads[2].wait()
    values = dot(toks, vw[...])
    first_head = lax.axis_index("tp") * heads
    decays = []
    for h in range(heads):
        number = (jnp.zeros((1, size), jnp.int32) + (first_head + h)).astype(F32)
        decays.append(1.0 - jnp.exp2(-2.0 - 10.0 * number / (heads * n_tp - 1)))
    writes = []
    for p in range(parts):
        states[p].wait()
        for t in range(p * span, (p + 1) * span):
            for h in range(heads):
                at = 2 * h * rows + t
                new = decays[h] * state[t, h] + columns[:, at + rows : at + rows + 1] * values[
                    t : t + 1, h * size : (h + 1) * size
                ]
                fresh[t, h] = new
                readout[t : t + 1, h * size : (h + 1) * size] = jnp.sum(
                    columns[:, at : at + 1] * new, axis=0, keepdims=True
                )
        write = pltpu.make_async_copy(
            fresh.at[pl.ds(p * span, span)], state_out.at[pl.ds(p * span, span)], out_sem.at[p]
        )
        write.start()
        writes.append(write)
    late[0].wait()
    gating = dot(toks, gw[...])
    late[1].wait()
    total = None
    for h in range(heads):
        cols = slice(h * size, (h + 1) * size)
        mixed = (normalize(readout[:, cols], head_gain[:, cols]) * silu(gating[:, cols])).astype(BF16)
        term = dot(mixed, ow[cols, :])
        total = term if total is None else total + term
    share_out[...] = total.astype(BF16)
    for write in writes:
        write.wait()


def layer_kernel(
    n_ep, n_tp,
    share, tokens, ids, id_weights, first_gain, second_gain, side_gate,
    dg_h, du_h, dd_h, eg_h, eu_h, ed_h, sg_h, su_h, sd_h,
    out,
    dg, du, dd, eg, eu, ed, sg, su, sd,
    got1, gathered, normed, switches, routing, hid_d, hid_e, hid_s, own_sum, core_out, core_in,
    y_out, y_in, total_out, ep_in, final,
    w_sem, s1, r1, sr, rr, sa, ra, sy, ry, sc, rc, s3, r3, s4, r4, s5, r5, s6, r6,
):
    ep, tp = lax.axis_index("ep"), lax.axis_index("tp")
    rows, width = tokens.shape
    cw = width // n_tp
    n_y = n_tp // 2
    y, core = tp // 2, lax.rem(tp, 2)
    mate = y * 2 + 1 - core
    barrier = pltpu.get_barrier_semaphore()

    def greet_ep(d, _):
        pl.semaphore_signal(
            barrier, inc=1, device_id=(lax.rem(ep + d, n_ep), tp), device_id_type=MESH
        )
        return 0

    def greet_tp(d, _):
        pl.semaphore_signal(
            barrier, inc=1, device_id=(ep, lax.rem(tp + d, n_tp)), device_id_type=MESH
        )
        return 0

    lax.fori_loop(1, n_ep, greet_ep, 0)
    lax.fori_loop(1, n_tp, greet_tp, 0)
    wide = eg.shape[-1] != eg_h.shape[-1]
    if wide:
        unit_e, unit_s = eg_h.shape[-1], sg_h.shape[-1]
        eg_d, eu_d = eg.at[:, :, pl.ds(0, unit_e)], eg.at[:, :, pl.ds(unit_e, unit_e)]
        sg_d, su_d = sg.at[:, pl.ds(0, unit_s)], sg.at[:, pl.ds(unit_s, unit_s)]
    else:
        eg_d, eu_d, sg_d, su_d = eg, eu, sg, su

    def both(x, gate_ref, up_ref, index):
        if wide:
            pair = dot(x, gate_ref[index])
            middle = pair.shape[1] // 2
            return silu(pair[:, :middle]) * pair[:, middle:]
        return silu(dot(x, gate_ref[index])) * dot(x, up_ref[index])

    weights = [
        pltpu.make_async_copy(src, dst, w_sem.at[at])
        for at, (src, dst) in enumerate(
            ((dg_h, dg), (du_h, du), (eg_h, eg_d), (eu_h, eu_d), (sg_h, sg_d), (su_h, su_d), (dd_h, dd), (ed_h, ed), (sd_h, sd))
        )
    ]
    for at in (4, 5, 0, 1, 2, 3, 6, 7, 8):
        weights[at].start()

    def rows_of(i):
        return pl.ds(pl.multiple_of(i * rows, rows), rows)

    def cols_of(j):
        return pl.ds(pl.multiple_of(j * cw, cw), cw)

    number = lax.broadcasted_iota(jnp.int32, (LANES, rows), 0)
    columns = jnp.zeros((LANES, rows), F32)
    for k in range(ids.shape[0]):
        columns = columns + jnp.where(ids[k : k + 1, :] == number, id_weights[k : k + 1, :], 0.0)
    unit = (
        lax.broadcasted_iota(jnp.int32, (rows, rows), 0) == lax.broadcasted_iota(jnp.int32, (rows, rows), 1)
    ).astype(F32)
    mine = lax.dot_general(
        unit, columns, (((1,), (1,)), ((), ())), precision=lax.Precision.HIGHEST, preferred_element_type=F32
    )
    routing[rows_of(ep), :] = mine
    hid_s[...] = jnp.zeros_like(hid_s)
    pl.semaphore_wait(barrier, n_ep + n_tp - 2)

    def copy1(d):
        peer = lax.rem(tp + d, n_tp)
        return pltpu.make_async_remote_copy(
            src_ref=share.at[:, cols_of(peer)], dst_ref=got1.at[d], send_sem=s1.at[d], recv_sem=r1.at[d],
            device_id=(ep, peer), device_id_type=MESH,
        )

    def copy_routing(d):
        return pltpu.make_async_remote_copy(
            src_ref=routing.at[rows_of(ep)], dst_ref=routing.at[rows_of(ep)], send_sem=sr.at[d],
            recv_sem=rr.at[d], device_id=(lax.rem(ep + d, n_ep), tp), device_id_type=MESH,
        )

    def routing_from(d):
        origin = rows_of(lax.rem(ep - d + n_ep, n_ep))
        return pltpu.make_async_remote_copy(
            src_ref=routing.at[origin], dst_ref=routing.at[origin], send_sem=sr.at[d],
            recv_sem=rr.at[d], device_id=(lax.rem(ep + d, n_ep), tp), device_id_type=MESH,
        )

    def loop(low, high, action):
        def step(d, carry):
            action(d)
            return carry

        lax.fori_loop(low, high, step, 0)

    loop(1, n_tp, lambda d: copy1(d).start())
    loop(1, n_ep, lambda d: copy_routing(d).start())
    piece = RESIDUAL_SCALE * tokens[:, cols_of(tp)].astype(F32) + share[:, cols_of(tp)].astype(F32)
    for d in range(1, n_tp):
        copy1(d).wait_recv()
        piece = piece + got1[d].astype(F32)
    gathered[rows_of(ep), cols_of(tp)] = piece.astype(BF16)

    def block(i, j):
        return gathered.at[rows_of(i), cols_of(j)]

    def ag(d, origin):
        return pltpu.make_async_remote_copy(
            src_ref=block(origin, tp), dst_ref=block(origin, tp), send_sem=sa.at[d], recv_sem=ra.at[d],
            device_id=(lax.rem(ep + d, n_ep), tp), device_id_type=MESH,
        )

    def along_y(d, e, j):
        peer = lax.rem(y + e, n_y) * 2 + core
        origin = lax.rem(ep - d + n_ep, n_ep)
        return pltpu.make_async_remote_copy(
            src_ref=block(origin, j), dst_ref=block(origin, j), send_sem=sy.at[e - 1, d],
            recv_sem=ry.at[e - 1, d], device_id=(ep, peer), device_id_type=MESH,
        )

    def to_mate(d, e, side):
        origin = lax.rem(ep - d + n_ep, n_ep)
        j = lax.rem(y - e + n_y, n_y) * 2 + side
        return pltpu.make_async_remote_copy(
            src_ref=block(origin, j), dst_ref=block(origin, j), send_sem=sc.at[e, d],
            recv_sem=rc.at[e, d], device_id=(ep, mate), device_id_type=MESH,
        )

    loop(1, n_ep, lambda d: ag(d, ep).start())

    def pass_on(d):
        for e in range(1, n_y):
            along_y(d, e, tp).start()
        to_mate(d, 0, core).start()

    pass_on(0)

    def arrived(d):
        ag(d, lax.rem(ep - d + n_ep, n_ep)).wait_recv()
        pass_on(d)

    loop(1, n_ep, arrived)

    def over(d):
        for e in range(1, n_y):
            along_y(d, e, lax.rem(y - e + n_y, n_y) * 2 + core).wait_recv()
            to_mate(d, e, core).start()

    gain1 = first_gain[...]
    side = side_gate[...].astype(F32)
    side = jnp.concatenate([side[r : r + 1, :] for r in range(width // LANES)], axis=1)

    def finish(d):
        for e in range(n_y):
            to_mate(d, e, 1 - core).wait_recv()
        where = rows_of(lax.rem(ep - d + n_ep, n_ep))
        after = normalize(gathered[where, :].astype(F32), gain1).astype(BF16)
        normed[where, :] = after
        turned = jax.nn.sigmoid(jnp.sum(after.astype(F32) * side, axis=-1, keepdims=True))
        switches[where, :] = jnp.broadcast_to(turned, (rows, LANES))

    loop(0, n_ep - 2, over)
    finish(0)
    weights[4].wait()
    weights[5].wait()
    own = normed[rows_of(ep), :]
    hid_s[rows_of(ep), :] = both(own, sg, su, Ellipsis).astype(BF16)
    loop(n_ep - 2, n_ep, over)
    loop(1, n_ep, finish)
    loop(1, n_ep, lambda d: routing_from(d).wait_recv())

    everyone = normed[...]
    weights[0].wait()
    gate = dot(everyone, dg[...])
    weights[1].wait()
    up = dot(everyone, du[...])
    hid_d[...] = (silu(gate) * up * switches[:, 0:1]).astype(BF16)
    weights[2].wait()
    weights[3].wait()
    experts = eg.shape[0]
    lanes = lax.broadcasted_iota(jnp.int32, routing.shape, 1)
    for e in range(experts):
        weight = jnp.sum(
            jnp.where(lanes == ep * experts + e, routing[...], 0.0), axis=-1, keepdims=True
        )
        hidden = (both(everyone, eg, eu, e) * weight).astype(BF16)
        if wide:
            hid_e[0, :, e * unit_e : (e + 1) * unit_e] = hidden
        else:
            hid_e[e] = hidden
    for at in (6, 7, 8):
        weights[at].wait()

    near_ep = n_ep // 2
    half_rows = near_ep * rows
    near = ep // near_ep

    def half_of(s):
        which = near if s else 1 - near
        return pl.ds(pl.multiple_of(which * half_rows, half_rows), half_rows)

    def product(s, j):
        where, cols = half_of(s), cols_of(j)
        result = dot(hid_d[where, :], dd[:, cols]) + dot(hid_s[where, :], sd[:, cols])
        for e in range(ed.shape[0]):
            result = result + dot(hid_e[e, where, :], ed[e, :, cols])
        return result

    def core_copy(s, e):
        at = s * n_y + e
        return pltpu.make_async_remote_copy(
            src_ref=core_out.at[at], dst_ref=core_in.at[at], send_sem=s3.at[at], recv_sem=r3.at[at],
            device_id=(ep, mate), device_id_type=MESH,
        )

    def y_copy(s, e):
        at = s * (n_y - 1) + e - 1
        peer = lax.rem(y + e, n_y) * 2 + core
        return pltpu.make_async_remote_copy(
            src_ref=y_out.at[at], dst_ref=y_in.at[at], send_sem=s4.at[at], recv_sem=r4.at[at],
            device_id=(ep, peer), device_id_type=MESH,
        )

    def ep_copy(d):
        peer = lax.rem(ep + d, n_ep)
        return pltpu.make_async_remote_copy(
            src_ref=total_out.at[rows_of(peer)], dst_ref=ep_in.at[d], send_sem=s5.at[d],
            recv_sem=r5.at[d], device_id=(peer, tp), device_id_type=MESH,
        )

    def terms(s, e):
        target = lax.rem(y + e, n_y) * 2
        at = s * n_y + e
        core_out[at] = product(s, target + 1 - core).astype(BF16)
        core_copy(s, e).start()
        own_sum[s] = product(s, target + core)
        if e:
            core_copy(s, e).wait_recv()
            y_out[s * (n_y - 1) + e - 1] = (own_sum[s] + core_in[at].astype(F32)).astype(BF16)
            y_copy(s, e).start()

    def send_total(s):
        core_copy(s, 0).wait_recv()
        total = own_sum[s] + core_in[s * n_y].astype(F32)
        for e in range(1, n_y):
            y_copy(s, e).wait_recv()
            total = total + y_in[s * (n_y - 1) + e - 1].astype(F32)
        total_out[half_of(s), :] = total.astype(BF16)
        if s:
            base = near * near_ep
            inside = ep - base
            loop(1, near_ep, lambda m: ep_copy(lax.rem(base + lax.rem(inside + m, near_ep) - ep + n_ep, n_ep)).start())
        else:
            base = (1 - near) * near_ep
            loop(0, near_ep, lambda m: ep_copy(lax.rem(base + m - ep + n_ep, n_ep)).start())

    for e in range(1, n_y):
        terms(0, e)
    terms(0, 0)
    for e in range(1, n_y):
        terms(1, e)
    send_total(0)
    terms(1, 0)
    send_total(1)

    def gather_sum(d, so_far):
        ep_copy(d).wait_recv()
        return so_far + ep_in[d].astype(F32)

    mine = lax.fori_loop(1, n_ep, gather_sum, total_out[rows_of(ep), :].astype(F32))
    final[:, cols_of(tp)] = mine.astype(BF16)

    def last_copy(d, j):
        return pltpu.make_async_remote_copy(
            src_ref=final.at[:, cols_of(j)], dst_ref=final.at[:, cols_of(j)], send_sem=s6.at[d],
            recv_sem=r6.at[d], device_id=(ep, lax.rem(tp + d, n_tp)), device_id_type=MESH,
        )

    loop(1, n_tp, lambda d: last_copy(d, tp).start())
    loop(1, n_tp, lambda d: last_copy(d, lax.rem(tp - d + n_tp, n_tp)).wait_recv())
    result = RESIDUAL_SCALE * normed[rows_of(ep), :].astype(F32) + final[...].astype(F32)
    out[...] = normalize(result, second_gain[...]).astype(BF16)

    def settle(d):
        ag(d, ep).wait_send()
        copy_routing(d).wait_send()
        ep_copy(d).wait_send()

    loop(1, n_ep, settle)

    def settle_tp(d):
        copy1(d).wait_send()
        last_copy(d, tp).wait_send()

    loop(1, n_tp, settle_tp)

    def settle_forward(d):
        for e in range(n_y):
            to_mate(d, e, core).wait_send()
            if e:
                along_y(d, e, tp).wait_send()

    loop(0, n_ep, settle_forward)
    for s in range(2):
        for e in range(n_y):
            core_copy(s, e).wait_send()
            if e:
                y_copy(s, e).wait_send()


def per_device(
    n_ep, n_tp,
    tokens, lengths, old_state, query_weight, key_weight, value_weight, gate_weight, head_gain,
    output_weight, first_gain, expert_ids, expert_weights, expert_gate, expert_up, expert_down,
    shared_gate, shared_up, shared_down, side_gate, dense_gate, dense_up, dense_down, second_gain,
):
    rows, width = tokens.shape
    heads, size = old_state.shape[1], old_state.shape[-1]
    half = size // 2
    frequency = np.tile(10000.0 ** (-np.arange(half) * 2.0 / size), 2)[None].astype(np.float32)
    inner = heads * size
    vmem = pl.BlockSpec(memory_space=pltpu.VMEM)
    anywhere = pl.BlockSpec(memory_space=pl.ANY)
    parts = 4
    dma = pltpu.SemaphoreType.DMA
    share, new_state = pl.pallas_call(
        functools.partial(mixer_kernel, n_tp),
        out_shape=(
            jax.ShapeDtypeStruct((rows, width), BF16),
            jax.ShapeDtypeStruct(old_state.shape, F32),
        ),
        in_specs=[pl.BlockSpec(memory_space=pltpu.SMEM)] + [vmem] * 3 + [anywhere] * 6,
        out_specs=(vmem, anywhere),
        scratch_shapes=[pltpu.VMEM((width, inner), BF16)] * 4
        + [
            pltpu.VMEM((inner, width), BF16),
            pltpu.VMEM(old_state.shape, F32),
            pltpu.VMEM(old_state.shape, F32),
            pltpu.VMEM((rows, inner), F32),
            dma((5,)),
            dma((parts,)),
            dma((parts,)),
        ],
        name="mixer",
    )(
        lengths, tokens, jnp.asarray(frequency), head_gain.reshape(1, -1), old_state, query_weight, key_weight,
        value_weight, gate_weight, output_weight,
    )
    cw = width // n_tp
    n_y = n_tp // 2
    everyone = rows * n_ep
    experts, unit = expert_gate.shape[0], expert_gate.shape[2]
    wide = unit % LANES == 0
    if wide:
        expert_down = expert_down.reshape(1, experts * unit, width)
    big = [dense_gate, dense_up, dense_down, expert_gate, expert_up, expert_down, shared_gate, shared_up, shared_down]
    shapes = [w.shape for w in big]
    if wide:
        shapes[3], shapes[4] = (experts, width, 2 * unit), (16, LANES)
        shapes[6], shapes[7] = (width, 2 * shared_gate.shape[1]), (16, LANES)
    layer_out = pl.pallas_call(
        functools.partial(layer_kernel, n_ep, n_tp),
        out_shape=jax.ShapeDtypeStruct((rows, width), BF16),
        in_specs=[vmem] * 7 + [anywhere] * len(big),
        out_specs=vmem,
        scratch_shapes=[pltpu.VMEM(shape, BF16) for shape in shapes]
        + [
            pltpu.VMEM((n_tp, rows, cw), BF16),
            pltpu.VMEM((everyone, width), BF16),
            pltpu.VMEM((everyone, width), BF16),
            pltpu.VMEM((everyone, LANES), F32),
            pltpu.VMEM((everyone, LANES), F32),
            pltpu.VMEM((everyone, dense_gate.shape[1]), BF16),
            pltpu.VMEM((expert_down.shape[0], everyone, expert_down.shape[1]), BF16),
            pltpu.VMEM((everyone, shared_gate.shape[1]), BF16),
            pltpu.VMEM((2, everyone // 2, cw), F32),
            pltpu.VMEM((2 * n_y, everyone // 2, cw), BF16),
            pltpu.VMEM((2 * n_y, everyone // 2, cw), BF16),
            pltpu.VMEM((2 * (n_y - 1), everyone // 2, cw), BF16),
            pltpu.VMEM((2 * (n_y - 1), everyone // 2, cw), BF16),
            pltpu.VMEM((everyone, cw), BF16),
            pltpu.VMEM((n_ep, rows, cw), BF16),
            pltpu.VMEM((rows, width), BF16),
            dma((len(big),)),
        ]
        + [dma((n_tp,))] * 2
        + [dma((n_ep,))] * 4
        + [dma((n_y - 1, n_ep))] * 2
        + [dma((n_y, n_ep))] * 2
        + [dma((2 * n_y,))] * 2
        + [dma((2 * (n_y - 1),))] * 2
        + [dma((n_ep,))] * 2
        + [dma((n_tp,))] * 2,
        compiler_params=pltpu.CompilerParams(collective_id=0, has_side_effects=True),
        name="layer",
    )(
        share, tokens, expert_ids.T, expert_weights.T, first_gain.reshape(1, -1),
        second_gain.reshape(1, -1), side_gate.reshape(-1, LANES), *big,
    )
    return layer_out, new_state


def solution(mesh):
    return jax.shard_map(
        functools.partial(per_device, mesh.shape["ep"], mesh.shape["tp"]),
        mesh=mesh,
        in_specs=(
            P("ep", None),
            P("ep"),
            P("ep", "tp", None, None),
            P(None, "tp"),
            P(None, "tp"),
            P(None, "tp"),
            P(None, "tp"),
            P("tp"),
            P("tp", None),
            P(),
            P("ep", None),
            P("ep", None),
            P("ep", None, "tp"),
            P("ep", None, "tp"),
            P("ep", "tp", None),
            P(None, "tp"),
            P(None, "tp"),
            P("tp", None),
            P(),
            P(None, ("ep", "tp")),
            P(None, ("ep", "tp")),
            P(("ep", "tp"), None),
            P(),
        ),
        out_specs=(P("ep", None), P("ep", "tp", None, None)),
        check_vma=False,
    )
```
